32 devices in a mesh: grp: 2 (over y), ep: 4 (over z), tp: 4 (over x, core).
Axes of the slice: x: 2, y: 2, z: 4, core: 2. Of those that a mesh axis runs over, the one named last changes fastest.
Arguments:
- x_in: bfloat16 [512, 2048], P(('grp', 'ep')), parts along dimension 0, may hold values from -6 to 6
- state: float32 [512, 96, 128], P(('grp', 'ep'), 'tp'), parts along dimension 0, may hold values from -6 to 6
- routes: int32 [512, 2], P(('grp', 'ep')), parts along dimension 0, may hold values from 0 to 7, as said below
- w_in: bfloat16 [2048, 1536], P(None, 'tp'), may hold values from -0.125 to 0.125
- decay_rate: float32 [96, 64], P('tp'), may hold values from 0.01 to 1
- frequency: float32 [96, 64], P('tp'), may hold values from 0 to 192
- log_step: float32 [96], P('tp'), may hold values from -3 to 0
- b_in: float32 [96, 16, 128], P('tp'), may hold values from -1.5 to 1.5
- c_out: float32 [96, 16, 128], P('tp'), may hold values from -0.5 to 0.5
- skip: float32 [1536], P('tp'), may hold values from -3 to 3
- w_out: bfloat16 [1536, 2048], P('tp'), may hold values from -0.15625 to 0.15625
- gain_mix: float32 [2048], replicated, may hold values from 0.1 to 1.9
- w_group: bfloat16 [2048, 4], replicated, may hold values from -0.0625 to 0.0625
- w_expert: bfloat16 [2048, 8], replicated, may hold values from -0.0625 to 0.0625
- w_gate: bfloat16 [8, 2048, 1024], P('ep', None, 'tp'), may hold values from -0.125 to 0.125
- w_up: bfloat16 [8, 2048, 1024], P('ep', None, 'tp'), may hold values from -0.125 to 0.125
- w_down: bfloat16 [8, 1024, 2048], P('ep', 'tp'), may hold values from -3 to 3
- gain_moe: float32 [2048], replicated, may hold values from 0.1 to 1.9
Outputs:
- layer_out: bfloat16 [512, 2048], P(('grp', 'ep')), parts along dimension 0
- new_state: float32 [512, 96, 128], P(('grp', 'ep'), 'tp'), parts along dimension 0
The draws below stay inside these ranges and needn't reach their ends.
There are 2 independent parts, one for each index of `grp`. The reference program is written for one: setup_inputs(seed, part) draws one part's arguments, and reference() takes and returns one part's arrays. A program takes and returns all parts, laid end to end along the dimension named above; an argument that names none is the same for every part. Nothing has to cross between parts.
Inputs may be any that keep to these rules, and one draw needn't show every extreme that they name: `routes`: each row names two different experts of one group of 2 consecutive expert numbers. Within the rows of one index of ep (aligned blocks of 64 rows) no expert is named by more than 32 rows, and in every block some expert is named by exactly 32 rows.
All inputs are finite; a program needn't handle non-finite values.
Results may differ from the reference program's by a relative error of at most 0.015.
Values may be sent and summed in bfloat16 or wider, within the bound.
A program may use at most 64 MiB of HBM per device.

```python
import math
import jax
import jax.numpy as jnp
from jax import lax

D = 2048
MIX = 1536
GROUP = 16
CHGROUPS = 96
STATE = 64
MIX_DEV = 384
FF = 1024
FF_DEV = 256
TOP = 2
EXPERTS = 8
EGROUPS = 4
SEQ_DEV = 64
SEQS = 256
CAP = 32
N_EP = 4
N_TP = 4


def shuffle_rows(key_row):
    return jax.random.permutation(key_row, SEQ_DEV).astype(jnp.int32)


def shuffle_group(key_group):
    return jax.random.permutation(key_group, EXPERTS // EGROUPS).astype(jnp.int32)


def draw_routes(key, part):
    block_count = SEQS // SEQ_DEV
    pair_count = EXPERTS // 2
    group_size = EXPERTS // EGROUPS
    key_pair, key_order, key_offset, key_rows = jax.random.split(key, 4)
    within = jax.vmap(shuffle_group)(jax.random.split(key_pair, EGROUPS))
    members = within + group_size * jnp.arange(EGROUPS, dtype=jnp.int32)[:, None]
    pair_table = members.reshape(pair_count, 2)
    pair_order = jax.random.permutation(key_order, pair_count).astype(jnp.int32)
    offsets = jax.random.randint(key_offset, (block_count, 1), 0, pair_count - 1).astype(jnp.int32)
    ranks = jnp.arange(SEQ_DEV, dtype=jnp.int32)[None, :]
    slot_pick = jnp.where(ranks < CAP, 0, 1 + (ranks - CAP + offsets) % (pair_count - 1))
    slot_pick = jnp.broadcast_to(slot_pick, (block_count, SEQ_DEV))
    shuffled = jax.vmap(shuffle_rows)(jax.random.split(key_rows, block_count))
    mixed_pick = jnp.take_along_axis(slot_pick, shuffled, axis=1)
    picked = pair_table[pair_order[mixed_pick]]
    return picked.reshape(SEQS, 2).astype(jnp.int32)


def steps_of(key, shape, cuts, smallest, top_value):
    loudness, own = 1.0, jax.random.fold_in(key, 6)
    for axis_at, shards_of in cuts:
        steps = jnp.exp(jax.random.uniform(jax.random.fold_in(own, axis_at), (shards_of,), jnp.float32, smallest / len(cuts), top_value / len(cuts)))
        loudness = loudness * jnp.repeat(steps, shape[axis_at] // shards_of).reshape([-1 if axis == axis_at else 1 for axis in range(len(shape))])
    return loudness


def noise(stream_key, dims, scale, bound, shards=(), held_as=jnp.bfloat16):
    result = jax.random.normal(stream_key, dims, jnp.float32) * scale
    if len(shards) > 0:
        result = steps_of(stream_key, dims, shards, -0.22, 0.18) * result
    return jnp.clip(result, min=-bound, max=bound).astype(held_as)


def setup_inputs(seed: int = 0, part: int = 0) -> dict:
    seeds = jax.random.split(jax.random.key(seed), 19)
    part_splits = jax.random.split(jax.random.fold_in(seeds[18], part), 19)
    return {
        "x_in": noise(part_splits[0], (SEQS, D), 1.0, 6.0, ((0, 4),)),
        "state": noise(part_splits[1], (SEQS, CHGROUPS, 2 * STATE), 1.0, 6.0, ((0, 4), (1, 4)), jnp.float32),
        "routes": draw_routes(jax.random.fold_in(jax.random.fold_in(seeds[18], part), 71), part),
        "w_in": noise(seeds[3], (D, MIX), D ** -0.5, 0.125, ((1, 4),)),
        "decay_rate": jnp.clip(jnp.exp(math.log(1.0) - 4.6051702 * jax.random.uniform(seeds[4], (CHGROUPS, STATE), jnp.float32) ** steps_of(seeds[4], (CHGROUPS, STATE), ((0, 4),), -0.2, 0.2)), 0.01, 1.0),
        "frequency": jnp.clip(192.0 * jax.random.uniform(seeds[5], (CHGROUPS, STATE), jnp.float32) ** steps_of(seeds[5], (CHGROUPS, STATE), ((0, 4),), -0.2, 0.2), 0.0, 192.0),
        "log_step": jnp.clip(-3.0 + 3.0 * jax.random.uniform(seeds[6], (CHGROUPS,), jnp.float32) ** steps_of(seeds[6], (CHGROUPS,), ((0, 4),), -0.2, 0.2), -3.0, 0.0),
        "b_in": noise(seeds[7], (CHGROUPS, GROUP, 2 * STATE), GROUP ** -0.5, 1.5, ((0, 4),), jnp.float32),
        "c_out": noise(seeds[8], (CHGROUPS, GROUP, 2 * STATE), (2 * STATE) ** -0.5, 0.5, ((0, 4),), jnp.float32),
        "skip": noise(seeds[9], (MIX,), 0.5, 3.0, ((0, 4),), jnp.float32),
        "w_out": noise(seeds[10], (MIX, D), MIX ** -0.5, 0.15625, ((0, 4),)),
        "gain_mix": jnp.clip(1.0 + 0.18 * jax.random.normal(seeds[11], (D,), jnp.float32), 0.1, 1.9),
        "w_group": noise(seeds[12], (D, EGROUPS), (4 * D) ** -0.5, 0.0625),
        "w_expert": noise(seeds[13], (D, EXPERTS), (4 * D) ** -0.5, 0.0625),
        "w_gate": noise(seeds[14], (EXPERTS, D, FF), D ** -0.5, 0.125, ((0, 4), (2, 4))),
        "w_up": noise(seeds[15], (EXPERTS, D, FF), D ** -0.5, 0.125, ((0, 4), (2, 4))),
        "w_down": noise(seeds[16], (EXPERTS, FF, D), (max(1, FF // 256)) ** -0.5, 3.0, ((0, 4), (1, 4))),
        "gain_moe": jnp.clip(1.0 + 0.18 * jax.random.normal(seeds[17], (D,), jnp.float32), 0.1, 1.9),
    }


residual_scale = 8.0 ** 0.25
norm_eps = 1e-05

def normalize(values, gain):
    centre = lax.optimization_barrier(jnp.mean(values, -1, keepdims=True))
    spread = lax.optimization_barrier(jnp.mean(jnp.square(values - centre), -1, keepdims=True))
    return (values - centre) * lax.rsqrt(spread + norm_eps) * gain

def s5_advance(mix_input, state, decay_rate, frequency, log_step, b_in, c_out, skip):
    top_precision = lax.Precision.HIGHEST
    entries = decay_rate.shape[-1]
    group_count = decay_rate.shape[0]
    width = b_in.shape[1]
    seq_count = mix_input.shape[0]
    input_rows = mix_input.astype(jnp.float32).reshape(seq_count, group_count, width)
    step_size = jnp.exp(log_step)[:, None]
    lam_real = -decay_rate
    lam_imag = frequency
    magnitude = jnp.exp(lam_real * step_size)
    angle_dt = lam_imag * step_size
    bar_real = magnitude * jnp.cos(angle_dt)
    bar_imag = magnitude * jnp.sin(angle_dt)
    minus_real = bar_real - 1.0
    modulus = lam_real * lam_real + lam_imag * lam_imag
    ratio_real = (minus_real * lam_real + bar_imag * lam_imag) / modulus
    ratio_imag = (bar_imag * lam_real - minus_real * lam_imag) / modulus
    in_real = b_in[..., :entries]
    in_imag = b_in[..., entries:]
    input_matrix_real = ratio_real[:, None, :] * in_real - ratio_imag[:, None, :] * in_imag
    input_matrix_imag = ratio_real[:, None, :] * in_imag + ratio_imag[:, None, :] * in_real
    forcing_real = jnp.einsum('rxf,xfb->rxb', input_rows, input_matrix_real, precision=top_precision)
    forcing_imag = jnp.einsum('rxf,xfb->rxb', input_rows, input_matrix_imag, precision=top_precision)
    old_real = state[..., :entries]
    old_imag = state[..., entries:]
    following_real = bar_real * old_real - bar_imag * old_imag + forcing_real
    following_imag = bar_real * old_imag + bar_imag * old_real + forcing_imag
    output_real = c_out[..., :entries]
    output_imag = c_out[..., entries:]
    output_matrix = jnp.einsum('lzt,zft->lzf', following_real, output_real, precision=top_precision)
    output_matrix = output_matrix - jnp.einsum('lzt,zft->lzf', following_imag, output_imag, precision=top_precision)
    output_matrix = output_matrix + skip.reshape(group_count, width) * input_rows
    activated = jax.nn.gelu(output_matrix).reshape(seq_count, group_count * width)
    return (activated, jnp.concatenate([following_real, following_imag], axis=-1))

def route_weights(normed, routes, w_group, w_expert):
    group_total = w_group.shape[1]
    expert_total = w_expert.shape[1]
    per_group = expert_total // group_total
    group_logit = jnp.dot(normed, w_group, preferred_element_type=jnp.float32)
    group_exp = jnp.exp(group_logit)
    group_prob = group_exp / lax.optimization_barrier(jnp.sum(group_exp, -1, keepdims=True))
    chosen = routes[:, 0] // per_group
    group_pick = lax.optimization_barrier(jnp.sum(jnp.where(chosen[:, None] == jnp.arange(group_total, dtype=jnp.int32)[None, :], group_prob, 0.0), -1))
    expert_logit = jnp.dot(normed, w_expert, preferred_element_type=jnp.float32)
    picked = lax.optimization_barrier(jnp.sum(jnp.where(routes[:, :, None] == jnp.arange(expert_total, dtype=jnp.int32)[None, None, :], expert_logit[:, None, :], 0.0), -1))
    pair_exp = jnp.exp(picked)
    return pair_exp / lax.optimization_barrier(jnp.sum(pair_exp, -1, keepdims=True)) * group_pick[:, None]

def reference(x_in, state, routes, w_in, decay_rate, frequency, log_step, b_in, c_out, skip, w_out, gain_mix, w_group, w_expert, w_gate, w_up, w_down, gain_moe):
    mix_input = jnp.dot(x_in, w_in, preferred_element_type=jnp.float32).astype(jnp.bfloat16)
    activated, new_state = s5_advance(mix_input, state, decay_rate, frequency, log_step, b_in, c_out, skip)
    mix_act = activated.astype(jnp.bfloat16)
    block_parts = jnp.einsum('ntc,tcd->ntd', mix_act.astype(jnp.float32).reshape(SEQS, N_TP, MIX_DEV), w_out.astype(jnp.float32).reshape(N_TP, MIX_DEV, D))
    block_parts = lax.optimization_barrier(block_parts.astype(jnp.bfloat16))
    mixed = lax.optimization_barrier(jnp.sum(block_parts.astype(jnp.float32), axis=1))
    hidden_state = normalize(residual_scale * x_in.astype(jnp.float32) + mixed, gain_mix)
    hidden_bf = hidden_state.astype(jnp.bfloat16)
    route_weight = route_weights(hidden_bf, routes, w_group, w_expert)
    block_routes = routes.reshape(N_EP, SEQ_DEV, TOP)
    hits = (block_routes[..., None] == jnp.arange(EXPERTS, dtype=jnp.int32)).astype(jnp.int32)
    tally = lax.optimization_barrier(jnp.sum(hits, axis=2))
    prior = jnp.cumsum(tally, axis=1) - tally
    slot_in_block = lax.optimization_barrier(jnp.sum(prior[:, :, None, :] * hits, axis=-1))
    block_index = jnp.arange(N_EP, dtype=jnp.int32)[:, None, None]
    position = (block_index * CAP + slot_in_block).reshape(-1).astype(jnp.int32)
    expert_flat = routes.reshape(-1).astype(jnp.int32)
    row_copies = jnp.broadcast_to(hidden_bf[:, None, :], (SEQS, TOP, D)).reshape(SEQS * TOP, D)
    buffer = jnp.zeros((EXPERTS, N_EP * CAP, D), jnp.bfloat16).at[expert_flat, position].set(row_copies)

    def one_expert(operands):
        slot_rows, gate_weight, up_weight, down_weight = operands
        gate_val = jnp.dot(slot_rows, gate_weight, preferred_element_type=jnp.float32)
        up_val = jnp.dot(slot_rows, up_weight, preferred_element_type=jnp.float32)
        act = (jax.nn.silu(gate_val) * up_val).astype(jnp.bfloat16)
        pieces = jnp.einsum('rtf,tfd->rtd', act.astype(jnp.float32).reshape(N_EP * CAP, N_TP, FF_DEV), down_weight.astype(jnp.float32).reshape(N_TP, FF_DEV, D))
        pieces = lax.optimization_barrier(pieces.astype(jnp.bfloat16))
        return lax.optimization_barrier(jnp.sum(pieces.astype(jnp.float32), axis=1)).astype(jnp.bfloat16)
    outputs = lax.map(one_expert, (buffer, w_gate, w_up, w_down))
    expert_out = outputs[expert_flat, position].reshape(SEQS, TOP, D).astype(jnp.float32)
    moe = lax.optimization_barrier(jnp.sum(route_weight[:, :, None] * expert_out, axis=1))
    layer_out = normalize(residual_scale * hidden_state + moe, gain_moe).astype(jnp.bfloat16)
    return (layer_out, new_state)
```

```python
import functools
import math

import jax
import jax.numpy as jnp
from jax import lax
from jax.experimental import pallas as pl
from jax.experimental.pallas import tpu as pltpu
from jax.sharding import PartitionSpec as P

residual_scale = 8.0**0.25
norm_eps = 1e-05


def normalize(values, gain):
    centre = jnp.mean(values, -1, keepdims=True)
    spread = jnp.mean(jnp.square(values - centre), -1, keepdims=True)
    return (values - centre) * lax.rsqrt(spread + norm_eps) * gain


def s5_advance(mix_input, state, decay_rate, frequency, log_step, b_in, c_out, skip):
    top_precision = lax.Precision.HIGHEST
    entries = decay_rate.shape[-1]
    group_count = decay_rate.shape[0]
    width = b_in.shape[1]
    seq_count = mix_input.shape[0]
    input_rows = mix_input.astype(jnp.float32).reshape(seq_count, group_count, width)
    step_size = jnp.exp(log_step)[:, None]
    lam_real = -decay_rate
    magnitude = jnp.exp(lam_real * step_size)
    angle_dt = frequency * step_size
    bar_real = magnitude * jnp.cos(angle_dt)
    bar_imag = magnitude * jnp.sin(angle_dt)
    minus_real = bar_real - 1.0
    modulus = lam_real * lam_real + frequency * frequency
    ratio_real = (minus_real * lam_real + bar_imag * frequency) / modulus
    ratio_imag = (bar_imag * lam_real - minus_real * frequency) / modulus
    in_real = b_in[..., :entries]
    in_imag = b_in[..., entries:]
    input_matrix_real = ratio_real[:, None, :] * in_real - ratio_imag[:, None, :] * in_imag
    input_matrix_imag = ratio_real[:, None, :] * in_imag + ratio_imag[:, None, :] * in_real
    forcing_real = jnp.einsum(
        "rxf,xfb->rxb", input_rows, input_matrix_real, precision=top_precision
    )
    forcing_imag = jnp.einsum(
        "rxf,xfb->rxb", input_rows, input_matrix_imag, precision=top_precision
    )
    old_real = state[..., :entries]
    old_imag = state[..., entries:]
    following_real = bar_real * old_real - bar_imag * old_imag + forcing_real
    following_imag = bar_real * old_imag + bar_imag * old_real + forcing_imag
    output_real = c_out[..., :entries]
    output_imag = c_out[..., entries:]
    output_matrix = jnp.einsum("lzt,zft->lzf", following_real, output_real, precision=top_precision)
    output_matrix = output_matrix - jnp.einsum(
        "lzt,zft->lzf", following_imag, output_imag, precision=top_precision
    )
    output_matrix = output_matrix + skip.reshape(group_count, width) * input_rows
    activated = jax.nn.gelu(output_matrix).reshape(seq_count, group_count * width)
    return (activated, jnp.concatenate([following_real, following_imag], axis=-1))


def route_weights(normed, routes, w_group, w_expert):
    group_total = w_group.shape[1]
    expert_total = w_expert.shape[1]
    per_group = expert_total // group_total
    group_logit = jnp.dot(normed, w_group, preferred_element_type=jnp.float32)
    group_exp = jnp.exp(group_logit)
    group_prob = group_exp / jnp.sum(group_exp, -1, keepdims=True)
    chosen = routes[:, 0] // per_group
    group_pick = jnp.sum(
        jnp.where(
            chosen[:, None] == jnp.arange(group_total, dtype=jnp.int32)[None, :], group_prob, 0.0
        ),
        -1,
    )
    expert_logit = jnp.dot(normed, w_expert, preferred_element_type=jnp.float32)
    picked = jnp.sum(
        jnp.where(
            routes[:, :, None] == jnp.arange(expert_total, dtype=jnp.int32)[None, None, :],
            expert_logit[:, None, :],
            0.0,
        ),
        -1,
    )
    pair_exp = jnp.exp(picked)
    return pair_exp / jnp.sum(pair_exp, -1, keepdims=True) * group_pick[:, None]


def per_device(
    x_in,
    state,
    routes,
    w_in,
    decay_rate,
    frequency,
    log_step,
    b_in,
    c_out,
    skip,
    w_out,
    gain_mix,
    w_group,
    w_expert,
    w_gate,
    w_up,
    w_down,
    gain_moe,
):
    top_precision = lax.Precision.HIGHEST
    seq_count = x_in.shape[0]
    model_width = x_in.shape[1]
    mix_input = jnp.dot(x_in, w_in, preferred_element_type=jnp.float32).astype(jnp.bfloat16)
    activated, new_state = s5_advance(
        mix_input, state, decay_rate, frequency, log_step, b_in, c_out, skip
    )
    partial_mix = jnp.dot(activated.astype(jnp.bfloat16), w_out, preferred_element_type=jnp.float32)
    mixed = lax.psum(partial_mix.astype(jnp.bfloat16), "tp").astype(jnp.float32)
    hidden_state = normalize(residual_scale * x_in.astype(jnp.float32) + mixed, gain_mix)
    hidden_bf = hidden_state.astype(jnp.bfloat16)
    route_weight = route_weights(hidden_bf, routes, w_group, w_expert)
    expert_total = w_expert.shape[1]
    ep_count = lax.axis_size("ep")
    local_experts = w_gate.shape[0]
    capacity = max(2, 4 * seq_count // expert_total)
    total_slots = expert_total * capacity
    hits = (routes[:, :, None] == jnp.arange(expert_total, dtype=jnp.int32)[None, None, :]).astype(
        jnp.int32
    )
    tally = jnp.sum(hits, axis=1)
    prior = jnp.cumsum(tally, axis=0) - tally
    slot_in_block = jnp.sum(prior[:, None, :] * hits, axis=-1)
    target = routes * capacity + slot_in_block
    slot_ids = jnp.arange(total_slots, dtype=jnp.int32)
    matches = target[:, :, None] == slot_ids[None, None, :]
    dispatch_map = jnp.any(slot_ids[:, None, None] == target[None, :, :], axis=-1).astype(
        jnp.bfloat16
    )
    combine_map = jnp.sum(jnp.where(matches, route_weight[:, :, None], 0.0), axis=1)
    buffer = jnp.dot(dispatch_map, hidden_bf, preferred_element_type=jnp.float32).astype(
        jnp.bfloat16
    )
    buffer = buffer.reshape(ep_count, local_experts, capacity, model_width)
    slot_rows = lax.all_to_all(buffer, "ep", split_axis=0, concat_axis=0, tiled=True)
    gate_val = jnp.einsum("njcd,jdf->njcf", slot_rows, w_gate, preferred_element_type=jnp.float32)
    up_val = jnp.einsum("njcd,jdf->njcf", slot_rows, w_up, preferred_element_type=jnp.float32)
    act = (jax.nn.silu(gate_val) * up_val).astype(jnp.bfloat16)
    share = lax.psum_scatter(
        jnp.einsum("njcf,jfd->njcd", act, w_down, preferred_element_type=jnp.float32).astype(
            jnp.bfloat16
        ),
        "tp",
        scatter_dimension=3,
        tiled=True,
    )
    returned_rows = lax.all_to_all(share, "ep", split_axis=0, concat_axis=0, tiled=True)
    flat_rows = returned_rows.reshape(total_slots, returned_rows.shape[3])
    moe = jnp.dot(
        combine_map,
        lax.all_gather(flat_rows, "tp", axis=1, tiled=True).astype(jnp.float32),
        precision=top_precision,
    )
    layer_out = normalize(residual_scale * hidden_state + moe, gain_moe).astype(jnp.bfloat16)
    return (layer_out, new_state)


MESH = pl.DeviceIdType.MESH


def sin_cos(angle):
    turns = jnp.floor(angle * (2.0 / math.pi) + 0.5)
    rest = ((angle - turns * 1.5703125) - turns * 4.837512969970703e-4) - turns * 7.549789954891882e-8
    square = rest * rest
    sine = rest + rest * square * (
        -1.6666654611e-1 + square * (8.3321608736e-3 - square * 1.9515295891e-4)
    )
    cosine = (
        1.0
        - 0.5 * square
        + square
        * square
        * (4.166664568298827e-2 + square * (-1.388731625493765e-3 + square * 2.443315711809948e-5))
    )
    quadrant = turns - 4.0 * jnp.floor(turns * 0.25)
    odd = (quadrant == 1.0) | (quadrant == 3.0)
    swapped_sine = jnp.where(odd, cosine, sine)
    swapped_cosine = jnp.where(odd, sine, cosine)
    out_sine = jnp.where(quadrant >= 2.0, -swapped_sine, swapped_sine)
    flip = (quadrant == 1.0) | (quadrant == 2.0)
    out_cosine = jnp.where(flip, -swapped_cosine, swapped_cosine)
    return out_sine, out_cosine


def nt_dot(left, right):
    return lax.dot_general(
        left, right, (((1,), (1,)), ((), ())), preferred_element_type=jnp.float32
    )


def f32_dot(left, right):
    return jnp.dot(left, right, preferred_element_type=jnp.float32)


def to_lanes(columns, rows):
    lane = lax.broadcasted_iota(jnp.int32, (rows, 128), 1)
    packed = jnp.zeros((rows, 128), jnp.float32)
    for at, column in enumerate(columns):
        packed = jnp.where(lane == at, column, packed)
    if rows < 128:
        packed = jnp.concatenate([packed, jnp.zeros((128 - rows, 128), jnp.float32)], 0)
    return packed.T[0:8]


def to_columns(lines, rows):
    row = lax.broadcasted_iota(jnp.int32, (128, 128), 0)
    packed = jnp.zeros((128, 128), jnp.float32)
    for at, line in enumerate(lines):
        packed = jnp.where(row == at, line, packed)
    return packed.T[:rows]


def fused_kernel(
    log_hbm, x_hbm, state_hbm, routes_hbm, w_in_hbm, decay_hbm, freq_hbm, b_hbm, c_hbm, skip_hbm,
    w_out_hbm, gain_mix_hbm, w_group_hbm, w_expert_hbm, w_gate_hbm, w_up_hbm, w_down_hbm,
    gain_moe_hbm,
    out_ref, new_state,
    log_step, decay, freq, skip, routes, gain_mix, w_group, w_expert, gain_moe,
    x_ref, state, w_in, w_out, b_ref, c_ref, w_gate, w_up, w_down,
    b_blocks, c_blocks,
    mix_send, mix_recv, stat_mix, hidden_f32, go_rows, rows_all, line_all, line_columns,
    core_send, core_recv, cross_send, cross_recv, back_send, back_out, back_recv,
    out_parts, stat_out,
    local_sem,
    mix_ss, mix_rs, stat_ss, stat_rs, go_ss, go_rs, line_ss, line_rs, gather_ss, gather_rs,
    core_ss, core_rs, cross_ss, cross_rs, back_ss, back_rs,
    last_ss, last_rs, stat2_ss, stat2_rs,
):
    tp = lax.axis_index("tp")
    ep = lax.axis_index("ep")
    n_ep = lax.axis_size("ep")
    n_tp = 4
    seqs, width = x_ref.shape
    quarter = width // n_tp
    groups = decay.shape[0]
    entries = decay.shape[1]
    chans = b_ref.shape[0] // groups
    mix_dev = w_in.shape[1]
    cap = go_rows.shape[1]
    slots = n_ep * cap
    ff = w_gate.shape[2]
    experts = w_gate.shape[0]

    core = tp % 2
    chip = tp // 2
    peer = {
        0: tp,
        1: chip * 2 + (1 - core),
        2: (1 - chip) * 2 + core,
        3: (1 - chip) * 2 + (1 - core),
    }

    def tp_copy(src, dst, send_sem, recv_sem, k):
        return pltpu.make_async_remote_copy(
            src_ref=src, dst_ref=dst, send_sem=send_sem, recv_sem=recv_sem,
            device_id={"tp": peer[k]}, device_id_type=MESH,
        )

    def ep_copy(src, dst, send_sem, recv_sem, j):
        return pltpu.make_async_remote_copy(
            src_ref=src, dst_ref=dst, send_sem=send_sem, recv_sem=recv_sem,
            device_id={"ep": (ep + j) % n_ep}, device_id_type=MESH,
        )

    def columns(q):
        return pl.ds(pl.multiple_of(q * quarter, quarter), quarter)

    loads = {}
    for at, (name, src, dst) in enumerate((
        ("log", log_hbm, log_step), ("decay", decay_hbm, decay), ("freq", freq_hbm, freq),
        ("b", b_hbm, b_ref), ("c", c_hbm, c_ref), ("x", x_hbm, x_ref), ("w_in", w_in_hbm, w_in),
        ("skip", skip_hbm, skip), ("routes", routes_hbm, routes), ("gain_mix", gain_mix_hbm, gain_mix),
        ("state", state_hbm, state), ("w_out", w_out_hbm, w_out),
        ("w_group", w_group_hbm, w_group), ("w_expert", w_expert_hbm, w_expert),
        ("gain_moe", gain_moe_hbm, gain_moe),
        ("gate", w_gate_hbm, w_gate), ("up", w_up_hbm, w_up), ("down", w_down_hbm, w_down),
    )):
        loads[name] = pltpu.make_async_copy(src, dst, local_sem.at[at])
        loads[name].start()

    barrier = pltpu.get_barrier_semaphore()
    for k in (1, 2, 3):
        pl.semaphore_signal(barrier, inc=1, device_id={"tp": peer[k]}, device_id_type=MESH)
    for j in range(1, n_ep):
        pl.semaphore_signal(
            barrier, inc=1, device_id={"ep": (ep + j) % n_ep}, device_id_type=MESH
        )

    loads["log"].wait()
    loads["decay"].wait()
    loads["freq"].wait()
    own_group = lax.broadcasted_iota(jnp.int32, (groups, groups), 0) == lax.broadcasted_iota(
        jnp.int32, (groups, groups), 1
    )
    step_log = jnp.sum(jnp.where(own_group, log_step[...], 0.0), 1, keepdims=True)
    step_size = jnp.exp(step_log)
    lam_real = -decay[...]
    lam_imag = freq[...]
    magnitude = jnp.exp(lam_real * step_size)
    sine, cosine = sin_cos(lam_imag * step_size)
    bar_real = magnitude * cosine
    bar_imag = magnitude * sine
    minus_real = bar_real - 1.0
    modulus = lam_real * lam_real + lam_imag * lam_imag
    ratio_real = (minus_real * lam_real + bar_imag * lam_imag) / modulus
    ratio_imag = (bar_imag * lam_real - minus_real * lam_imag) / modulus
    bar_same = jnp.concatenate([bar_real, bar_real], 1)
    bar_cross = jnp.concatenate([-bar_imag, bar_imag], 1)
    ratio_same = jnp.concatenate([ratio_real, ratio_real], 1)
    ratio_cross = jnp.concatenate([-ratio_imag, ratio_imag], 1)
    lanes = 2 * entries
    per_block = b_blocks.shape[2] // lanes
    blocks = b_blocks.shape[0]
    b_blocks[...] = jnp.zeros_like(b_blocks)
    c_blocks[...] = jnp.zeros_like(c_blocks)
    loads["b"].wait()
    loads["c"].wait()
    sign = jnp.where(lax.broadcasted_iota(jnp.int32, (chans, lanes), 1) < entries, 1.0, -1.0)
    for g in range(groups):
        block, j = g // per_block, g % per_block
        b_in = b_ref[g * chans:(g + 1) * chans, :]
        b_bar = ratio_same[g:g + 1] * b_in + ratio_cross[g:g + 1] * pltpu.roll(b_in, entries, 1)
        rows = slice(j * chans, (j + 1) * chans)
        cols = slice(j * lanes, (j + 1) * lanes)
        b_blocks[block, rows, cols] = b_bar.astype(jnp.bfloat16)
        c_blocks[block, rows, cols] = (
            c_ref[g * chans:(g + 1) * chans, :] * sign
        ).astype(jnp.bfloat16)

    loads["x"].wait()
    loads["w_in"].wait()
    mix_input = f32_dot(x_ref[...], w_in[...]).astype(jnp.bfloat16)
    loads["state"].wait()
    loads["skip"].wait()
    block_chans = per_block * chans
    activated = []
    for block in range(blocks):
        chan = slice(block * block_chans, (block + 1) * block_chans)
        inputs = mix_input[:, chan]
        forcing = f32_dot(inputs, b_blocks[block])
        following = []
        for j in range(per_block):
            g = block * per_block + j
            old = state[pl.ds(g, seqs, stride=groups), :]
            new = (
                bar_same[g:g + 1] * old
                + bar_cross[g:g + 1] * pltpu.roll(old, entries, 1)
                + forcing[:, j * lanes:(j + 1) * lanes]
            )
            new_state[pl.ds(g, seqs, stride=groups), :] = new
            following.append(new.astype(jnp.bfloat16))
        mixed = nt_dot(jnp.concatenate(following, 1), c_blocks[block])
        mixed = mixed + skip[block:block + 1, :] * inputs.astype(jnp.float32)
        inner = math.sqrt(2.0 / math.pi) * (mixed + 0.044715 * mixed * mixed * mixed)
        activated.append((0.5 * mixed * (1.0 + jnp.tanh(inner))).astype(jnp.bfloat16))
    activated = jnp.concatenate(activated, 1)

    for name in ("w_out", "routes", "gain_mix", "w_group", "w_expert", "gain_moe"):
        loads[name].wait()
    pl.semaphore_wait(barrier, 2 + n_ep)
    mix_copies = {}
    for k in (2, 3, 1):
        mix_send[k - 1] = f32_dot(activated, w_out[:, columns(peer[k])]).astype(jnp.bfloat16)
        mix_copies[k] = tp_copy(
            mix_send.at[k - 1], mix_recv.at[k - 1], mix_ss.at[k - 1], mix_rs.at[k - 1], k
        )
        mix_copies[k].start()
    own = f32_dot(activated, w_out[:, columns(tp)]).astype(jnp.bfloat16).astype(jnp.float32)
    per_group = w_expert.shape[0] // w_group.shape[0]
    chosen = routes[0:1, :] // per_group
    group_rows = -(-n_ep // 8) * 8
    in_group = jnp.where(
        chosen == lax.broadcasted_iota(jnp.int32, (group_rows, seqs), 0), 1.0, 0.0
    )
    earlier = jnp.where(
        lax.broadcasted_iota(jnp.int32, (seqs, seqs), 0)
        < lax.broadcasted_iota(jnp.int32, (seqs, seqs), 1),
        1.0,
        0.0,
    ).astype(jnp.bfloat16)
    prior = f32_dot(in_group.astype(jnp.bfloat16), earlier)
    rank = jnp.sum(prior * in_group, 0, keepdims=True)
    target = chosen.astype(jnp.float32) * cap + rank
    slot_row = lax.broadcasted_iota(jnp.int32, (slots, seqs), 0).astype(jnp.float32)
    slot_rows = jnp.where(target == slot_row, 1.0, 0.0)
    padded = slot_rows
    if seqs < slots:
        padded = jnp.concatenate(
            [slot_rows, jnp.zeros((slots, slots - seqs), jnp.float32)], 1
        )
    slot_map = padded.T.astype(jnp.bfloat16)
    slot_rows = slot_rows.astype(jnp.bfloat16)

    value = residual_scale * x_ref[:, columns(tp)].astype(jnp.float32) + own
    for k in (1, 2, 3):
        mix_copies[k].wait_recv()
        value = value + mix_recv[k - 1].astype(jnp.float32)

    def share_stats(value, buffer, send_sem, recv_sem, send_rows):
        mean = jnp.mean(value, -1, keepdims=True)
        centred = value - mean
        send_rows(centred.astype(jnp.bfloat16))
        square = jnp.sum(centred * centred, -1, keepdims=True)
        buffer[tp] = to_lanes([mean, square], seqs)
        copies = []
        for k in (2, 3, 1):
            copies.append(
                tp_copy(buffer.at[tp], buffer.at[tp], send_sem.at[k - 1], recv_sem.at[k - 1], k)
            )
            copies[-1].start()
        return centred, mean, copies

    def total_stats(buffer, copies):
        for copy in copies:
            copy.wait_recv()
        parts = [buffer[q] for q in range(n_tp)]
        means = [part[0:1] for part in parts]
        mean = sum(means) * (1.0 / n_tp)
        square = sum(part[1:2] for part in parts)
        square = square + quarter * sum((m - mean) * (m - mean) for m in means)
        return means, mean, lax.rsqrt(square * (1.0 / width) + norm_eps)

    if n_ep == 4:
        half = ep // 2
        targets = [3 * (1 - half), 2 - half, 1 - ep + 4 * half, ep]
    else:
        targets = [(ep + j) % n_ep for j in range(1, n_ep)] + [ep]
    nearest = targets[n_ep - 2::-1]

    go_copies = []

    def send_centred(rows):
        packed = f32_dot(slot_rows, rows).astype(jnp.bfloat16)
        for d in range(n_ep):
            go_rows[d] = packed[d * cap:(d + 1) * cap]
        for source in nearest:
            go_copies.append(
                pltpu.make_async_remote_copy(
                    src_ref=go_rows.at[source], dst_ref=rows_all.at[tp, ep],
                    send_sem=go_ss.at[source], recv_sem=go_rs.at[ep],
                    device_id={"ep": source}, device_id_type=MESH,
                )
            )
            go_copies[-1].start()

    centred, mean_own, mix_stat_copies = share_stats(
        value, stat_mix, stat_ss, stat_rs, send_centred
    )

    gather_sends = []

    def gather(source, way, k, q, piece):
        copy = tp_copy(
            piece, rows_all.at[q, source], gather_ss.at[way, source], gather_rs.at[way, source], k
        )
        copy.start()
        gather_sends.append(copy)

    def gather_wait(source, way, q):
        tp_copy(
            rows_all.at[q, source], rows_all.at[q, source],
            gather_ss.at[way, source], gather_rs.at[way, source], 1,
        ).wait_recv()

    rows_all[tp, ep] = go_rows[ep]
    gather(ep, 1, 2, tp, go_rows.at[ep])
    gather(ep, 0, 1, tp, go_rows.at[ep])
    means, mean, scale = total_stats(stat_mix, mix_stat_copies)
    line_row = lax.broadcasted_iota(jnp.int32, (8, 128), 0)
    lines = jnp.where(line_row == n_tp, scale, 0.0)
    for q in range(n_tp):
        lines = jnp.where(line_row == q, means[q] - mean, lines)
    split = []
    for _ in range(3):
        split.append(lines.astype(jnp.bfloat16))
        lines = lines - split[-1].astype(jnp.float32)
    split = f32_dot(jnp.concatenate([p.astype(jnp.float32) for p in split], 0).astype(jnp.bfloat16), slot_map)
    line_all[ep] = split[0:8] + split[8:16] + split[16:24]
    line_copies = []
    for j in (2, 1, 3) if n_ep == 4 else range(1, n_ep):
        line_copies.append(
            ep_copy(line_all.at[ep], line_all.at[ep], line_ss.at[j - 1], line_rs.at[j - 1], j)
        )
        line_copies[-1].start()
    back = to_columns([mean, scale], seqs)
    hidden_f32[...] = (centred + (mean_own - back[:, 0:1])) * back[:, 1:2] * gain_mix[:, columns(tp)]
    for source in nearest:
        ep_copy(
            go_rows.at[0], rows_all.at[tp, source], go_ss.at[source], go_rs.at[source], 1
        ).wait_recv()
        gather(source, 1, 2, tp, rows_all.at[tp, source])
        gather(source, 0, 1, tp, rows_all.at[tp, source])
    for source in [ep] + nearest:
        gather_wait(source, 1, peer[2])
        gather(source, 2, 1, peer[2], rows_all.at[peer[2], source])
    loads["gate"].wait()
    loads["up"].wait()
    loads["down"].wait()
    for source in [ep] + nearest:
        gather_wait(source, 0, peer[1])
        gather_wait(source, 2, peer[3])

    for j in range(1, n_ep):
        source = (ep + n_ep - j) % n_ep
        ep_copy(
            line_all.at[ep], line_all.at[source], line_ss.at[j - 1], line_rs.at[j - 1], j
        ).wait_recv()
    lines = [line_all[source] for source in range(n_ep)]
    if 8 * n_ep < 128:
        lines.append(jnp.zeros((128 - 8 * n_ep, 128), jnp.float32))
    line_columns[...] = jnp.concatenate(lines, 0).T
    mine = line_columns[pl.ds(pl.multiple_of(ep * cap, cap), cap), :]

    def line_column(at):
        return jnp.concatenate([mine[:, 8 * d + at:8 * d + at + 1] for d in range(n_ep)], 0)

    scale = line_column(n_tp)
    row_list = []
    for q in range(n_tp):
        part = rows_all[q].reshape(slots, quarter).astype(jnp.float32) + line_column(q)
        gain = gain_mix[:, q * quarter:(q + 1) * quarter]
        row_list.append((part * scale * gain).astype(jnp.bfloat16))
    row_list = jnp.concatenate(row_list, 1)
    group_logit = nt_dot(row_list, w_group[...])
    group_logit = group_logit - jnp.max(group_logit, -1, keepdims=True)
    group_exp = jnp.exp(group_logit)
    mine = lax.broadcasted_iota(jnp.int32, group_logit.shape, 1) == ep
    group_prob = jnp.sum(jnp.where(mine, group_exp, 0.0), -1, keepdims=True) / jnp.sum(
        group_exp, -1, keepdims=True
    )
    expert_logit = nt_dot(row_list, w_expert[...])
    expert_lane = lax.broadcasted_iota(jnp.int32, expert_logit.shape, 1)
    picked = [
        jnp.sum(jnp.where(expert_lane == ep * experts + e, expert_logit, 0.0), -1, keepdims=True)
        for e in range(experts)
    ]
    highest = functools.reduce(jnp.maximum, picked)
    picked = [jnp.exp(p - highest) for p in picked]
    share = group_prob / sum(picked)
    acts = []
    for e in range(experts):
        gate_val = f32_dot(row_list, w_gate[e])
        up_val = f32_dot(row_list, w_up[e])
        silu = gate_val * (0.5 + 0.5 * jnp.tanh(0.5 * gate_val))
        acts.append((silu * up_val * (picked[e] * share)).astype(jnp.bfloat16))
    acts = jnp.concatenate(acts, 1)

    core_copies = []
    for at, k in enumerate((3, 1)):
        core_send[at] = f32_dot(acts, w_down[:, columns(peer[k])]).astype(jnp.bfloat16)
        core_copies.append(
            tp_copy(core_send.at[at], core_recv.at[at], core_ss.at[at], core_rs.at[at], 1)
        )
        core_copies[-1].start()
    across = f32_dot(acts, w_down[:, columns(peer[2])])
    core_copies[0].wait_recv()
    cross_send[...] = (
        (across + core_recv[0].astype(jnp.float32)).astype(jnp.bfloat16).reshape(n_ep, cap, quarter)
    )
    cross_copies = {}
    for j, source in enumerate(targets):
        cross_copies[j] = tp_copy(
            cross_send.at[source], cross_recv.at[source],
            cross_ss.at[source], cross_rs.at[source], 2,
        )
        cross_copies[j].start()
    own = f32_dot(acts, w_down[:, columns(tp)])
    core_copies[1].wait_recv()
    back_send[...] = (own + core_recv[1].astype(jnp.float32)).reshape(n_ep, cap, quarter)
    back_copies = {}
    for j, source in enumerate(targets):
        cross_copies[j].wait_recv()
        total = (back_send[source] + cross_recv[source].astype(jnp.float32)).astype(jnp.bfloat16)
        if j == n_ep - 1:
            back_recv[ep] = total
        else:
            back_out[source] = total
            back_copies[j] = pltpu.make_async_remote_copy(
                src_ref=back_out.at[source], dst_ref=back_recv.at[ep],
                send_sem=back_ss.at[source], recv_sem=back_rs.at[ep],
                device_id={"ep": source}, device_id_type=MESH,
            )
            back_copies[j].start()
    for j in range(1, n_ep):
        source = (ep + n_ep - j) % n_ep
        ep_copy(
            back_out.at[0], back_recv.at[source], back_ss.at[source], back_rs.at[source], j
        ).wait_recv()

    moe = f32_dot(slot_map[:seqs], back_recv[...].reshape(slots, quarter))
    value = residual_scale * hidden_f32[...] + moe
    def last(way, k, q):
        copy = tp_copy(out_parts.at[q], out_parts.at[q], last_ss.at[way], last_rs.at[way], k)
        copy.start()
        return copy

    def last_wait(way, q):
        tp_copy(out_parts.at[q], out_parts.at[q], last_ss.at[way], last_rs.at[way], 1).wait_recv()

    last_copies = []

    def send_last(rows):
        out_parts[tp] = rows
        last_copies.extend([last(1, 2, tp), last(0, 1, tp)])

    _, _, out_stat_copies = share_stats(value, stat_out, stat2_ss, stat2_rs, send_last)
    last_wait(1, peer[2])
    last_copies.append(last(2, 1, peer[2]))
    means, mean, scale = total_stats(stat_out, out_stat_copies)
    back = to_columns([scale] + [m - mean for m in means], seqs)
    last_wait(0, peer[1])
    last_wait(2, peer[3])
    for q in range(n_tp):
        part = out_parts[q].astype(jnp.float32) + back[:, q + 1:q + 2]
        cols = slice(q * quarter, (q + 1) * quarter)
        out_ref[:, cols] = (part * back[:, 0:1] * gain_moe[:, cols]).astype(jnp.bfloat16)

    sent = list(mix_copies.values()) + mix_stat_copies + go_copies + line_copies + gather_sends
    sent += core_copies + list(cross_copies.values()) + list(back_copies.values())
    for copy in sent + out_stat_copies + last_copies:
        copy.wait_send()


def store_kernel(out_in, state_in, out_ref, state_ref, store):
    stores = [
        pltpu.make_async_copy(state_in, state_ref, store.at[0]),
        pltpu.make_async_copy(out_in, out_ref, store.at[1]),
    ]
    for copy in stores:
        copy.start()
    for copy in stores:
        copy.wait()


def fused_device(
    x_in, state, routes, w_in, decay_rate, frequency, log_step, b_in, c_out, skip, w_out,
    gain_mix, w_group, w_expert, w_gate, w_up, w_down, gain_moe,
):
    seqs, width = x_in.shape
    groups, chans, lanes = b_in.shape
    mix_dev = w_in.shape[1]
    experts, _, ff = w_gate.shape
    n_ep = lax.axis_size("ep")
    n_tp = 4
    quarter = width // n_tp
    cap = max(2, 4 * seqs // w_expert.shape[1])
    per_block = 128 // chans
    blocks = groups // per_block
    bf16, f32 = jnp.bfloat16, jnp.float32
    vmem = pl.BlockSpec(memory_space=pltpu.VMEM)
    hbm = pl.BlockSpec(memory_space=pl.ANY)
    dma = pltpu.SemaphoreType.DMA
    layer_out, new_state = pl.pallas_call(
        fused_kernel,
        out_shape=(
            pltpu.VMEM((seqs, width), bf16),
            pltpu.VMEM((seqs * groups, lanes), f32),
        ),
        in_specs=[hbm] * 18,
        out_specs=(vmem, vmem),
        scratch_shapes=[
            pltpu.VMEM((1, groups), f32),
            pltpu.VMEM(decay_rate.shape, f32),
            pltpu.VMEM(decay_rate.shape, f32),
            pltpu.VMEM((blocks, mix_dev // blocks), f32),
            pltpu.VMEM((2, seqs), jnp.int32),
            pltpu.VMEM((1, width), f32),
            pltpu.VMEM((w_group.shape[1], width), bf16),
            pltpu.VMEM((w_expert.shape[1], width), bf16),
            pltpu.VMEM((1, width), f32),
            pltpu.VMEM((seqs, width), bf16),
            pltpu.VMEM((seqs * groups, lanes), f32),
            pltpu.VMEM(w_in.shape, bf16),
            pltpu.VMEM(w_out.shape, bf16),
            pltpu.VMEM((groups * chans, lanes), f32),
            pltpu.VMEM((groups * chans, lanes), f32),
            pltpu.VMEM(w_gate.shape, bf16),
            pltpu.VMEM(w_up.shape, bf16),
            pltpu.VMEM((experts * ff, width), bf16),
            pltpu.VMEM((blocks, per_block * chans, per_block * lanes), bf16),
            pltpu.VMEM((blocks, per_block * chans, per_block * lanes), bf16),
            pltpu.VMEM((3, seqs, quarter), bf16),
            pltpu.VMEM((3, seqs, quarter), bf16),
            pltpu.VMEM((n_tp, 8, 128), f32),
            pltpu.VMEM((seqs, quarter), f32),
            pltpu.VMEM((n_ep, cap, quarter), bf16),
            pltpu.VMEM((n_tp, n_ep, cap, quarter), bf16),
            pltpu.VMEM((n_ep, 8, 128), f32),
            pltpu.VMEM((128, 128), f32),
            pltpu.VMEM((2, n_ep * cap, quarter), bf16),
            pltpu.VMEM((2, n_ep * cap, quarter), bf16),
            pltpu.VMEM((n_ep, cap, quarter), bf16),
            pltpu.VMEM((n_ep, cap, quarter), bf16),
            pltpu.VMEM((n_ep, cap, quarter), f32),
            pltpu.VMEM((n_ep, cap, quarter), bf16),
            pltpu.VMEM((n_ep, cap, quarter), bf16),
            pltpu.VMEM((n_tp, seqs, quarter), bf16),
            pltpu.VMEM((n_tp, 8, 128), f32),
            dma((18,)),
            dma((3,)), dma((3,)), dma((3,)), dma((3,)),
            dma((n_ep,)), dma((n_ep,)), dma((n_ep - 1,)), dma((n_ep - 1,)),
            dma((3, n_ep)), dma((3, n_ep)),
            dma((2,)), dma((2,)),
            dma((n_ep,)), dma((n_ep,)), dma((n_ep,)), dma((n_ep,)),
            dma((3,)), dma((3,)), dma((3,)), dma((3,)),
        ],
        compiler_params=pltpu.CompilerParams(collective_id=0, has_side_effects=True),
    )(
        log_step.reshape(1, -1),
        x_in, state.reshape(seqs * groups, lanes), routes.T, w_in, decay_rate, frequency,
        b_in.reshape(groups * chans, lanes), c_out.reshape(groups * chans, lanes),
        skip.reshape(blocks, -1), w_out, gain_mix.reshape(1, -1), w_group.T, w_expert.T,
        w_gate, w_up, w_down.reshape(experts * ff, width), gain_moe.reshape(1, -1),
    )
    layer_out, new_state = pl.pallas_call(
        store_kernel,
        out_shape=(
            jax.ShapeDtypeStruct((seqs, width), bf16),
            jax.ShapeDtypeStruct((seqs * groups, lanes), f32),
        ),
        in_specs=[vmem, vmem],
        out_specs=(hbm, hbm),
        scratch_shapes=[dma((2,))],
    )(
        pltpu.with_memory_space_constraint(layer_out, pltpu.VMEM),
        pltpu.with_memory_space_constraint(new_state, pltpu.VMEM),
    )
    return layer_out, new_state.reshape(seqs, groups, lanes)


def device_step(*args):
    x_in, routes, b_in, w_group, w_expert, w_gate = (
        args[0], args[2], args[7], args[12], args[13], args[14]
    )
    seqs, width = x_in.shape
    groups, chans, lanes = b_in.shape
    n_ep = lax.axis_size("ep")
    experts = w_gate.shape[0]
    per_group = w_expert.shape[1] // w_group.shape[1]
    cap = max(2, 4 * seqs // w_expert.shape[1])
    fits = (
        lax.axis_size("tp") == 4
        and per_group == experts == routes.shape[1]
        and n_ep > 1
        and n_ep * cap == 128
        and cap % 16 == 0
        and seqs <= 128
        and seqs % 16 == 0
        and width % 512 == 0
        and lanes == 128
        and 128 % chans == 0
        and chans % 16 == 0
        and groups % (128 // chans) == 0
    )
    return fused_device(*args) if fits else per_device(*args)


def solution(mesh):
    in_specs = (
        P(("grp", "ep"), None),
        P(("grp", "ep"), "tp", None),
        P(("grp", "ep"), None),
        P(None, "tp"),
        P("tp", None),
        P("tp", None),
        P("tp"),
        P("tp", None, None),
        P("tp", None, None),
        P("tp"),
        P("tp", None),
        P(),
        P(),
        P(),
        P("ep", None, "tp"),
        P("ep", None, "tp"),
        P("ep", "tp", None),
        P(),
    )
    out_specs = (P(("grp", "ep"), None), P(("grp", "ep"), "tp", None))
    return jax.shard_map(
        device_step, mesh=mesh, in_specs=in_specs, out_specs=out_specs, check_vma=False
    )
```
